32 devices in a mesh: grp: 2 (over y), sp: 4 (over z), tp: 4 (over x, core).
Axes of the slice: x: 2, y: 2, z: 4, core: 2. Of those that a mesh axis runs over, the one named last changes fastest.
Arguments:
- queries: bfloat16 [4096, 1024], P(('grp', 'sp'), 'tp'), parts along dimension 0, may hold values from -6 to 6
- memory_keys: bfloat16 [4096, 1024], P(('grp', 'sp'), 'tp'), parts along dimension 0, may hold values from -6 to 6
- memory_values: bfloat16 [4096, 1024], P(('grp', 'sp'), 'tp'), parts along dimension 0, may hold values from -6 to 6
- output_preactivation: bfloat16 [4096, 1024], P(('grp', 'sp'), 'tp'), parts along dimension 0, may hold values from -12 to 12
- input_preactivation: float32 [8, 4096], P('tp', ('grp', 'sp')), parts along dimension 1, may hold values from -6 to 140
- forget_preactivation: float32 [8, 4096], P('tp', ('grp', 'sp')), parts along dimension 1, as said below
- extra_forget_terms: float32 [8, 4096], P('tp', ('grp', 'sp')), parts along dimension 1, may hold values from -1 to 0, as said below
- head_norm_gain: float32 [128], replicated, may hold values from 0.1 to 1.9
- output_projection_matrix: bfloat16 [1024, 2048], P('tp'), may hold values from -0.1875 to 0.1875
- residual: bfloat16 [4096, 2048], P(('grp', 'sp', 'tp')), parts along dimension 0, may hold values from -6 to 6
- feedforward_norm_gain: float32 [2048], replicated, may hold values from 0.1 to 1.9
- feedforward_up_matrix: bfloat16 [2048, 8192], P('sp', 'tp'), may hold values from -0.125 to 0.125
- feedforward_down_matrix: bfloat16 [8192, 2048], P('tp', 'sp'), may hold values from -0.0625 to 0.0625
Outputs:
- layer_out: bfloat16 [4096, 2048], P(('grp', 'sp', 'tp')), parts along dimension 0
The draws below stay inside these ranges and needn't reach their ends.
There are 2 independent parts, one for each index of `grp`. The reference program is written for one: setup_inputs(seed, part) draws one part's arguments, and reference() takes and returns one part's arrays. A program takes and returns all parts, laid end to end along the dimension named above; an argument that names none is the same for every part. Nothing has to cross between parts.
Inputs may be any that keep to these rules, and one draw needn't show every extreme that they name: `forget_preactivation`: forget gate pre-activations. `extra_forget_terms`: extra log forget terms, zero at most positions.
All inputs are finite; a program needn't handle non-finite values.
Results may differ from the reference program's by a relative error of at most 0.018.
Values may be sent and summed in bfloat16 or wider, within the bound.
A program may use at most 64 MiB of HBM per device.

```python
import math
import jax
import jax.numpy as jnp
from jax import lax

D = 2048
FF = 8192
H = 8
DH = 128
BLOCK = 128
TOK_DEV = 512
M_WIDTH = 1024
SEQ = 2048
N_TP = 4


def draw_input_preactivation(key, part):
    draws = jax.random.split(jax.random.fold_in(key, 11), 1)
    values = jnp.clip(jax.random.normal(draws[0], (H, SEQ), jnp.float32), -6.0, 6.0)
    return values


def draw_forget_preactivation(key, part):
    draws = jax.random.split(jax.random.fold_in(key, 23), 3)
    order = jax.random.permutation(draws[0], H)
    slowly = order < H // 2
    center = jnp.where(slowly, math.log(2.5 * SEQ), 4.0).astype(jnp.float32)
    shifts = jax.random.uniform(draws[1], (H, SEQ // TOK_DEV, 1), jnp.float32, -0.7, 0.7)
    shifts = jnp.broadcast_to(shifts, (H, SEQ // TOK_DEV, TOK_DEV)).reshape(H, SEQ)
    jitter = jax.random.uniform(draws[2], (H, SEQ), jnp.float32, -1.0, 1.0)
    return center[:, None] + shifts + jitter


def draw_extra_forget_terms(key, part):
    draws = jax.random.split(jax.random.fold_in(key, 37), 2)
    quarter = SEQ // 4
    spots = jnp.arange(4)[None, :] * quarter + jax.random.randint(draws[0], (H, 4), 0, quarter)
    depths = jnp.log(jax.random.uniform(draws[1], (H, 4), jnp.float32, 0.5, 0.8))
    hits = jnp.arange(SEQ)[None, None, :] == spots[:, :, None]
    return jnp.sum(jnp.where(hits, depths[:, :, None], 0.0), axis=1)


def steps_of(stream_key, extent, cuts, low, top_value):
    gain, own = 1.0, jax.random.fold_in(stream_key, 6)
    for position, shards_of in cuts:
        steps = jnp.exp(jax.random.uniform(jax.random.fold_in(own, position), (shards_of,), jnp.float32, low / len(cuts), top_value / len(cuts)))
        gain = gain * jnp.repeat(steps, extent[position] // shards_of).reshape([-1 if axis == position else 1 for axis in range(len(extent))])
    return gain


def scatter_about(rng, shape, scale, reach, cuts=(), held_as=jnp.bfloat16):
    result = jax.random.normal(rng, shape, jnp.float32) * scale
    if len(cuts) > 0:
        result = steps_of(rng, shape, cuts, -0.22, 0.18) * result
    return jnp.clip(result, min=-reach, max=reach).astype(held_as)


def setup_inputs(seed: int = 0, part: int = 0) -> dict:
    key_of = jax.random.split(jax.random.key(seed), 14)
    part_splits = jax.random.split(jax.random.fold_in(key_of[13], part), 14)
    return {
        "queries": scatter_about(part_splits[0], (SEQ, M_WIDTH), 1.0, 6.0, ((0, 4), (1, 4))),
        "memory_keys": scatter_about(part_splits[1], (SEQ, M_WIDTH), 1.0, 6.0, ((0, 4), (1, 4))),
        "memory_values": scatter_about(part_splits[2], (SEQ, M_WIDTH), 1.0, 6.0, ((0, 4), (1, 4))),
        "output_preactivation": scatter_about(part_splits[3], (SEQ, M_WIDTH), 2.0, 12.0, ((0, 4), (1, 4))),
        "input_preactivation": draw_input_preactivation(jax.random.fold_in(jax.random.fold_in(key_of[13], part), 71), part),
        "forget_preactivation": draw_forget_preactivation(jax.random.fold_in(jax.random.fold_in(key_of[13], part), 71), part),
        "extra_forget_terms": draw_extra_forget_terms(jax.random.fold_in(jax.random.fold_in(key_of[13], part), 71), part),
        "head_norm_gain": jnp.clip(1.0 + 0.18 * jax.random.normal(key_of[7], (DH,), jnp.float32), 0.1, 1.9),
        "output_projection_matrix": scatter_about(key_of[8], (M_WIDTH, D), M_WIDTH ** -0.5, 0.1875, ((0, 4),)),
        "residual": scatter_about(part_splits[9], (SEQ, D), 1.0, 6.0, ((0, 16),)),
        "feedforward_norm_gain": jnp.clip(1.0 + 0.18 * jax.random.normal(key_of[10], (D,), jnp.float32), 0.1, 1.9),
        "feedforward_up_matrix": scatter_about(key_of[11], (D, FF), D ** -0.5, 0.125, ((0, 4), (1, 4))),
        "feedforward_down_matrix": scatter_about(key_of[12], (FF, D), FF ** -0.5, 0.0625, ((0, 4), (1, 4))),
    }


neg_big = -1e+30
norm_eps = 1e-06
highest = lax.Precision.HIGHEST

def rms_norm(tensor, gain_vec):
    mean_sq = lax.optimization_barrier(jnp.mean(tensor * tensor, axis=-1, keepdims=True))
    return tensor * lax.rsqrt(mean_sq + norm_eps) * gain_vec

def memory_cell(queries, memory_keys, memory_values, input_preactivation, forget_logarithm):
    blocks = SEQ // BLOCK

    def to_blocks(tensor):
        return jnp.moveaxis(tensor.reshape((H, blocks, BLOCK) + tensor.shape[2:]), 1, 0)
    causal = jnp.arange(BLOCK)[:, None] >= jnp.arange(BLOCK)[None, :]

    def advance(state_now, pieces):
        memory, stab_max = state_now
        query_blk, key_blk, val_blk, gate_blk, fgt_blk = pieces
        decay_logarithm = jnp.cumsum(fgt_blk, axis=-1)
        log_weight = decay_logarithm[:, :, None] - decay_logarithm[:, None, :] + gate_blk[:, None, :]
        log_weight = jnp.where(causal, log_weight, neg_big)
        carry_log = decay_logarithm + stab_max[:, None]
        row_max = jnp.maximum(lax.optimization_barrier(jnp.max(log_weight, axis=-1)), carry_log)
        scores = jnp.einsum('htd,hsd->hts', query_blk, key_blk, precision=highest) * jnp.exp(log_weight - row_max[..., None])
        carry_scale = jnp.exp(carry_log - row_max)
        hidden = jnp.einsum('hts,hsv->htv', scores, val_blk, precision=highest)
        hidden = hidden + carry_scale[..., None] * jnp.einsum('hvk,htk->htv', memory, query_blk, precision=highest)
        block_total = decay_logarithm[:, -1]
        tail_log = block_total[:, None] - decay_logarithm + gate_blk
        new_max = jnp.maximum(block_total + stab_max, lax.optimization_barrier(jnp.max(tail_log, axis=-1)))
        weights = jnp.exp(tail_log - new_max[:, None])
        carry_decay = jnp.exp(block_total + stab_max - new_max)
        memory = carry_decay[:, None, None] * memory + jnp.einsum('hs,hsv,hsk->hvk', weights, val_blk, key_blk, precision=highest)
        return ((memory, new_max), hidden)
    start_state = (jnp.zeros((H, DH, DH), jnp.float32), jnp.zeros((H,), jnp.float32))
    pieces = (to_blocks(queries), to_blocks(memory_keys), to_blocks(memory_values), to_blocks(input_preactivation), to_blocks(forget_logarithm))
    _, results = lax.scan(advance, start_state, pieces)
    return jnp.moveaxis(results, 0, 1).reshape(H, SEQ, DH)

def to_heads(tensor):
    return tensor.astype(jnp.float32).reshape(SEQ, H, DH).transpose(1, 0, 2)

def reference(queries, memory_keys, memory_values, output_preactivation, input_preactivation, forget_preactivation, extra_forget_terms, head_norm_gain, output_projection_matrix, residual, feedforward_norm_gain, feedforward_up_matrix, feedforward_down_matrix):
    forget_logarithm = jax.nn.log_sigmoid(forget_preactivation) + extra_forget_terms
    hidden = memory_cell(to_heads(queries), to_heads(memory_keys) * DH ** (-0.5), to_heads(memory_values), input_preactivation, forget_logarithm)
    hidden = hidden.transpose(1, 0, 2)
    gated = rms_norm(hidden, head_norm_gain) * jax.nn.sigmoid(output_preactivation.astype(jnp.float32).reshape(SEQ, H, DH))
    mixed = gated.reshape(SEQ, H * DH).astype(jnp.bfloat16)
    width_tp = H * DH // N_TP
    branch = jnp.zeros((SEQ, D), jnp.float32)
    for group_idx in range(N_TP):
        lower_col = group_idx * width_tp
        partial_value = jnp.dot(mixed[:, lower_col:lower_col + width_tp], output_projection_matrix[lower_col:lower_col + width_tp], preferred_element_type=jnp.float32)
        branch = branch + lax.optimization_barrier(partial_value.astype(jnp.bfloat16)).astype(jnp.float32)
    mid_state = (residual.astype(jnp.float32) + branch).astype(jnp.bfloat16)
    normed = rms_norm(mid_state.astype(jnp.float32), feedforward_norm_gain).astype(jnp.bfloat16)
    ff_tp = FF // N_TP
    mlp_sum = jnp.zeros((SEQ, D), jnp.float32)
    for group_idx in range(N_TP):
        lower_col = group_idx * ff_tp
        upward = jnp.dot(normed, feedforward_up_matrix[:, lower_col:lower_col + ff_tp], preferred_element_type=jnp.float32)
        active = jnp.square(jax.nn.relu(upward)).astype(jnp.bfloat16)
        partial_value = jnp.dot(active, feedforward_down_matrix[lower_col:lower_col + ff_tp], preferred_element_type=jnp.float32)
        mlp_sum = mlp_sum + lax.optimization_barrier(partial_value.astype(jnp.bfloat16)).astype(jnp.float32)
    return (mid_state.astype(jnp.float32) + mlp_sum).astype(jnp.bfloat16)
```

```python
import functools

import jax
import jax.numpy as jnp
from jax import lax
from jax.experimental import pallas as pl
from jax.experimental.pallas import tpu as pltpu
from jax.sharding import PartitionSpec as P

BLOCK = 128
EPS = 1e-06
NEG = -1e30
MESH = pl.DeviceIdType.MESH
F32 = jnp.float32
BF16 = jnp.bfloat16


def split_dot(exact, wide, swap=False):
    high = wide.astype(BF16)
    low = (wide - high.astype(F32)).astype(BF16)
    if swap:
        return jnp.dot(high, exact, preferred_element_type=F32) + jnp.dot(
            low, exact, preferred_element_type=F32
        )
    return jnp.dot(exact, high, preferred_element_type=F32) + jnp.dot(
        exact, low, preferred_element_type=F32
    )


def kernel(
    dims,
    q_ref, k_ref, v_ref, o_ref, arow_ref, acol_ref, ccol_ref, hgain_ref, wout_ref, res_ref,
    fgain_ref, up_ref, down_ref,
    mid_ref, mlp_ref,
    upw, dnw, ntok, act, msend, mrecv, bsend, brecv, mixed, blockmem, st_out, st_in,
    w_send, w_recv, loc_sem, st_send, st_recv, b_send, b_recv, t_send, t_recv, f_send, m_send, m_recv,
):
    grp, sp, tp, heads, blocks, rows = dims
    g, z, t = lax.axis_index("grp"), lax.axis_index("sp"), lax.axis_index("tp")
    layer = grp * tp
    me = g * tp + t
    half = tp // 2
    chunks = upw.shape[1]

    def there(gg, zz, tt):
        return {"grp": gg, "sp": zz, "tp": tt}

    barrier = pltpu.get_barrier_semaphore()
    for j in range(1, layer):
        d = lax.rem(me + j, layer)
        pl.semaphore_signal(
            barrier, inc=1, device_id=there(d // tp, z, lax.rem(d, tp)), device_id_type=MESH
        )

    @pl.when(z > 0)
    def _():
        pl.semaphore_signal(barrier, inc=1, device_id=there(g, z - 1, t), device_id_type=MESH)

    @pl.when(z < sp - 1)
    def _():
        pl.semaphore_signal(barrier, inc=1, device_id=there(g, z + 1, t), device_id_type=MESH)

    neighbours = (z + sp - 1) // sp + (2 * sp - 2 - z) // sp
    pl.semaphore_wait(barrier, layer - 1 + neighbours)

    hidden_half = up_ref.shape[1] // grp
    bufs = (upw, dnw)

    def own_piece(m, c):
        n = bufs[m].shape[2]
        if m == 0:
            return up_ref.at[
                pl.ds(c * n, n), pl.ds(pl.multiple_of(g * hidden_half, 128), hidden_half)
            ]
        return down_ref.at[pl.ds(pl.multiple_of(g * hidden_half + c * n, 16), n), :]

    def weight_copy(m, c, origin, way, source=None):
        dst = bufs[m].at[origin, c]
        zz = z + 1 if way == 0 else z - 1
        return pltpu.make_async_remote_copy(
            src_ref=dst if source is None else source,
            dst_ref=dst,
            send_sem=w_send.at[m, way, origin, c],
            recv_sem=w_recv.at[m, origin, c],
            device_id=there(g, zz, t),
            device_id_type=MESH,
        )

    def local_copy(m, c):
        return pltpu.make_async_copy(own_piece(m, c), bufs[m].at[z, c], loc_sem.at[m, c])

    def start_own(m):
        for c in range(chunks):
            @pl.when(z < sp - 1)
            def _():
                weight_copy(m, c, z, 0, own_piece(m, c)).start()

            @pl.when(z > 0)
            def _():
                weight_copy(m, c, z, 1, own_piece(m, c)).start()

    def relay(m, s):
        left, right = z - 1 - s, z + 1 + s
        for c in range(chunks):
            @pl.when(left >= 0)
            def _():
                weight_copy(m, c, left, 0).wait_recv()

                @pl.when(z < sp - 1)
                def _():
                    weight_copy(m, c, left, 0).start()

            @pl.when(right < sp)
            def _():
                weight_copy(m, c, right, 1).wait_recv()

                @pl.when(z > 0)
                def _():
                    weight_copy(m, c, right, 1).start()

    def relays(m, first, last):
        def body(s, _):
            relay(m, s)
            return 0

        lax.fori_loop(first, last, body, 0)

    start_own(0)
    for m in range(2):
        for c in range(chunks):
            local_copy(m, c).start()

    scale = BLOCK ** (-0.5) if q_ref.shape[1] // heads == BLOCK else (q_ref.shape[1] // heads) ** (-0.5)
    dh = q_ref.shape[1] // heads
    totals, tails = {}, {}
    for h in range(heads):
        cols = pl.ds(h * dh, dh)
        run = None
        for b in range(blocks):
            at = pl.ds(b * BLOCK, BLOCK)
            cum = ccol_ref[at, h : h + 1]
            total = cum[BLOCK - 1 : BLOCK, :]
            tail = total + acol_ref[at, h : h + 1]
            tail_max = jnp.max(tail, axis=0, keepdims=True)
            weighted = v_ref[at, cols].astype(F32) * jnp.exp(tail - tail_max)
            key_t = k_ref[at, cols].astype(F32).T.astype(BF16)
            mem = split_dot(key_t, weighted) * scale
            blockmem[h, b] = mem
            totals[h, b], tails[h, b] = total, tail_max
            if run is None:
                run = (total, tail_max, mem)
            else:
                new = jnp.maximum(total + run[1], tail_max)
                run = (
                    total + run[0],
                    new,
                    jnp.exp(total + run[1] - new) * run[2] + jnp.exp(tail_max - new) * mem,
                )
        st_out[h, :dh, :] = run[2]
        st_out[h, dh : dh + 8, :] = jnp.broadcast_to(run[1], (8, dh))
        st_out[h, dh + 8 : dh + 16, :] = jnp.broadcast_to(run[0], (8, dh))

    def state_copy():
        return pltpu.make_async_remote_copy(
            src_ref=st_out,
            dst_ref=st_in,
            send_sem=st_send,
            recv_sem=st_recv,
            device_id=there(g, z + 1, t),
            device_id_type=MESH,
        )

    @pl.when(z == 0)
    def _():
        st_in[...] = jnp.zeros_like(st_in)

    @pl.when(z > 0)
    def _():
        state_copy().wait_recv()

    @pl.when(z < sp - 1)
    def _():
        for h in range(heads):
            m_in = st_in[h, dh : dh + 1, :]
            m_loc = st_out[h, dh : dh + 1, :]
            total = st_out[h, dh + 8 : dh + 9, :]
            new = jnp.maximum(total + m_in, m_loc)
            st_out[h, :dh, :] = (
                jnp.exp(total + m_in - new) * st_in[h, :dh, :]
                + jnp.exp(m_loc - new) * st_out[h, :dh, :]
            )
            st_out[h, dh : dh + 8, :] = jnp.broadcast_to(new, (8, dh))
        state_copy().start()

    third = (sp - 1) // 3
    relays(0, 0, third)

    causal = lax.broadcasted_iota(jnp.int32, (BLOCK, BLOCK), 0) >= lax.broadcasted_iota(
        jnp.int32, (BLOCK, BLOCK), 1
    )
    gain = hgain_ref[...]
    for h in range(heads):
        cols = pl.ds(h * dh, dh)
        memory = st_in[h, :dh, :]
        stab = st_in[h, dh : dh + 1, 0:1]
        for b in range(blocks):
            at = pl.ds(b * BLOCK, BLOCK)
            cum = ccol_ref[at, h : h + 1]
            query = q_ref[at, cols]
            key_t = k_ref[at, cols].astype(F32).T.astype(BF16)
            log_weight = jnp.where(causal, cum + arow_ref[h * blocks + b : h * blocks + b + 1, :], NEG)
            carry = cum + stab
            row_max = jnp.maximum(jnp.max(log_weight, axis=1, keepdims=True), carry)
            scores = (
                jnp.dot(query, key_t, preferred_element_type=F32)
                * scale
                * jnp.exp(log_weight - row_max)
            )
            hidden = split_dot(v_ref[at, cols], scores, swap=True)
            hidden = hidden + jnp.exp(carry - row_max) * split_dot(query, memory)
            mean_sq = jnp.mean(hidden * hidden, axis=1, keepdims=True)
            gate = o_ref[at, cols].astype(F32)
            out = hidden * lax.rsqrt(mean_sq + EPS) * gain * (1.0 / (1.0 + jnp.exp(-gate)))
            mixed[at, cols] = out.astype(BF16)
            total, tail_max = totals[h, b], tails[h, b]
            new = jnp.maximum(total + stab, tail_max)
            memory = jnp.exp(total + stab - new) * memory + jnp.exp(tail_max - new) * blockmem[h, b]
            stab = new

    def branch_copy(j):
        d = lax.rem(t + j, tp)
        return pltpu.make_async_remote_copy(
            src_ref=bsend.at[j],
            dst_ref=brecv.at[j],
            send_sem=b_send.at[j],
            recv_sem=b_recv.at[j],
            device_id=there(g, z, d),
            device_id_type=MESH,
        )

    for j in list(range(1, tp)) + [0]:
        d = lax.rem(t + j, tp)
        part = jnp.dot(
            mixed[pl.ds(pl.multiple_of(d * rows, rows), rows), :],
            wout_ref[...],
            preferred_element_type=F32,
        )
        bsend[j] = part.astype(BF16)
        if j:
            branch_copy(j).start()

    branch = bsend[0].astype(F32)
    for j in range(1, tp):
        branch_copy(j).wait_recv()
        branch = branch + brecv[j].astype(F32)
    mid = (res_ref[...].astype(F32) + branch).astype(BF16)
    mid_ref[...] = mid
    wide = mid.astype(F32)
    mean_sq = jnp.mean(wide * wide, axis=1, keepdims=True)
    ntok[me] = (wide * lax.rsqrt(mean_sq + EPS) * fgain_ref[...]).astype(BF16)

    place = g * half + t // 2
    core = lax.rem(t, 2)
    same = grp * half

    def peer(j):
        there_at = lax.rem(place + j, same)
        return there_at // half, lax.rem(there_at, half) * 2 + core

    def token_copy(j, back=False):
        gg, tt = peer(j)
        slot = (gg * tp + tt) if back else me
        return pltpu.make_async_remote_copy(
            src_ref=ntok.at[slot],
            dst_ref=ntok.at[slot],
            send_sem=t_send.at[j],
            recv_sem=t_recv.at[slot],
            device_id=there(gg, z, tt),
            device_id_type=MESH,
        )

    def partner_copy(j, mine=True):
        gg, tt = peer(j)
        slot = gg * tp + (tt if mine else tt + 1 - 2 * core)
        return pltpu.make_async_remote_copy(
            src_ref=ntok.at[slot],
            dst_ref=ntok.at[slot],
            send_sem=f_send.at[j],
            recv_sem=t_recv.at[slot],
            device_id=there(g, z, t + 1 - 2 * core),
            device_id_type=MESH,
        )

    for j in range(1, same):
        token_copy(j).start()
    partner_copy(0).start()
    relays(0, third, 2 * third)
    start_own(1)
    for j in range(1, same):
        token_copy(j, back=True).wait_recv()
        partner_copy(j).start()
    for j in range(same):
        partner_copy(j, mine=False).wait_recv()
    relays(0, 2 * third, sp - 1)
    for m in range(2):
        for c in range(chunks):
            local_copy(m, c).wait()

    width = ntok.shape[2]
    pack = 2

    def up_step(i, _):
        x = ntok[pl.ds(i * pack, pack)].reshape(pack * rows, width)
        y = jnp.dot(x, upw[...].reshape(width, hidden_half), preferred_element_type=F32)
        y = jnp.maximum(y, 0.0)
        act[pl.ds(i * pack, pack)] = (y * y).astype(BF16).reshape(pack, rows, hidden_half)
        return 0

    lax.fori_loop(0, layer // pack, up_step, 0)

    out_cols = down_ref.shape[1]

    def mlp_copy(origin, j):
        d = lax.rem(me + j, layer)
        return pltpu.make_async_remote_copy(
            src_ref=msend.at[origin, j],
            dst_ref=mrecv.at[origin, j],
            send_sem=m_send.at[origin, j],
            recv_sem=m_recv.at[origin, j],
            device_id=there(d // tp, z, lax.rem(d, tp)),
            device_id_type=MESH,
        )

    def down_piece(origin):
        w = dnw[origin].reshape(hidden_half, out_cols)

        def step(i, _):
            j = layer - 1 - i
            x = act[lax.rem(me + j, layer)]
            msend[origin, j] = jnp.dot(x, w, preferred_element_type=F32).astype(BF16)

            @pl.when(j > 0)
            def _():
                mlp_copy(origin, j).start()

            return 0

        lax.fori_loop(0, layer, step, 0)

    down_piece(z)

    def down_step(s, _):
        relay(1, s)

        @pl.when(z - 1 - s >= 0)
        def _():
            down_piece(z - 1 - s)

        @pl.when(z + 1 + s < sp)
        def _():
            down_piece(z + 1 + s)

        return 0

    lax.fori_loop(0, sp - 1, down_step, 0)

    def finish(origin, _):
        total = msend[origin, 0].astype(F32)
        for j in range(1, layer):
            mlp_copy(origin, j).wait_recv()
            total = total + mrecv[origin, j].astype(F32)
        mlp_ref[origin] = total
        return 0

    lax.fori_loop(0, sp, finish, 0)

    def drain(origin, _):
        for j in range(1, layer):
            mlp_copy(origin, j).wait_send()
        for m in range(2):
            for c in range(chunks):
                @pl.when((origin <= z) & (z < sp - 1))
                def _():
                    weight_copy(m, c, origin, 0).wait_send()

                @pl.when((origin >= z) & (z > 0))
                def _():
                    weight_copy(m, c, origin, 1).wait_send()
        return 0

    lax.fori_loop(0, sp, drain, 0)
    for j in range(1, tp):
        branch_copy(j).wait_send()
    for j in range(1, same):
        token_copy(j).wait_send()
    for j in range(same):
        partner_copy(j).wait_send()

    @pl.when(z < sp - 1)
    def _():
        state_copy().wait_send()


def shards(
    mesh_shape,
    queries, memory_keys, memory_values, output_preactivation, input_preactivation,
    forget_preactivation, extra_forget_terms, head_norm_gain, output_projection_matrix, residual,
    feedforward_norm_gain, feedforward_up_matrix, feedforward_down_matrix,
):
    grp, sp, tp = mesh_shape
    tokens = queries.shape[0]
    heads = input_preactivation.shape[0]
    blocks = tokens // BLOCK
    dh = queries.shape[1] // heads
    rows, width = residual.shape
    layer = grp * tp
    up_rows, hidden = feedforward_up_matrix.shape
    hidden_half = hidden // grp
    out_cols = feedforward_down_matrix.shape[1]
    chunks = 2

    log_forget = jax.nn.log_sigmoid(forget_preactivation) + extra_forget_terms
    cum = jnp.cumsum(log_forget.reshape(heads, blocks, BLOCK), axis=-1)
    rest = input_preactivation.reshape(heads, blocks, BLOCK) - cum
    arow = rest.reshape(heads * blocks, BLOCK)
    acol = rest.reshape(heads, tokens).T
    ccol = cum.reshape(heads, tokens).T

    vmem = pl.BlockSpec(memory_space=pltpu.VMEM)
    hbm = pl.BlockSpec(memory_space=pl.ANY)
    dma = pltpu.SemaphoreType.DMA
    mid, mlp = pl.pallas_call(
        functools.partial(kernel, (grp, sp, tp, heads, blocks, rows)),
        out_shape=(
            jax.ShapeDtypeStruct((rows, width), BF16),
            jax.ShapeDtypeStruct((sp, rows, out_cols), F32),
        ),
        in_specs=[vmem] * 11 + [hbm] * 2,
        out_specs=(vmem, vmem),
        scratch_shapes=[
            pltpu.VMEM((sp, chunks, up_rows // chunks, hidden_half), BF16),
            pltpu.VMEM((sp, chunks, hidden_half // chunks, out_cols), BF16),
            pltpu.VMEM((layer, rows, width), BF16),
            pltpu.VMEM((layer, rows, hidden_half), BF16),
            pltpu.VMEM((sp, layer, rows, out_cols), BF16),
            pltpu.VMEM((sp, layer, rows, out_cols), BF16),
            pltpu.VMEM((tp, rows, width), BF16),
            pltpu.VMEM((tp, rows, width), BF16),
            pltpu.VMEM((tokens, heads * dh), BF16),
            pltpu.VMEM((heads, blocks, dh, dh), F32),
            pltpu.VMEM((heads, dh + 16, dh), F32),
            pltpu.VMEM((heads, dh + 16, dh), F32),
            dma((2, 2, sp, chunks)),
            dma((2, sp, chunks)),
            dma((2, chunks)),
            dma,
            dma,
            dma((tp,)),
            dma((tp,)),
            dma((layer,)),
            dma((layer,)),
            dma((layer,)),
            dma((sp, layer)),
            dma((sp, layer)),
        ],
        compiler_params=pltpu.CompilerParams(
            collective_id=0, has_side_effects=True, vmem_limit_bytes=60 * 1024 * 1024
        ),
    )(
        queries, memory_keys, memory_values, output_preactivation, arow, acol, ccol,
        head_norm_gain.reshape(1, dh), output_projection_matrix, residual,
        feedforward_norm_gain.reshape(1, width), feedforward_up_matrix, feedforward_down_matrix,
    )
    mlp = mlp.transpose(1, 0, 2).reshape(rows, width)
    return (mid.astype(F32) + mlp).astype(BF16)


def solution(mesh):
    in_specs = (
        P(("grp", "sp"), "tp"),
        P(("grp", "sp"), "tp"),
        P(("grp", "sp"), "tp"),
        P(("grp", "sp"), "tp"),
        P("tp", ("grp", "sp")),
        P("tp", ("grp", "sp")),
        P("tp", ("grp", "sp")),
        P(),
        P("tp", None),
        P(("grp", "sp", "tp"), None),
        P(),
        P("sp", "tp"),
        P("tp", "sp"),
    )
    out_specs = P(("grp", "sp", "tp"), None)
    shape = (mesh.shape["grp"], mesh.shape["sp"], mesh.shape["tp"])
    return jax.shard_map(
        functools.partial(shards, shape),
        mesh=mesh,
        in_specs=in_specs,
        out_specs=out_specs,
        check_vma=False,
    )
```

```python
import functools

import jax
import jax.numpy as jnp
from jax import lax
from jax.experimental import pallas as pl
from jax.experimental.pallas import tpu as pltpu
from jax.sharding import PartitionSpec as P

BLOCK = 128
EPS = 1e-06
NEG = -1e30
MESH = pl.DeviceIdType.MESH
F32 = jnp.float32
BF16 = jnp.bfloat16


def split_dot(exact, wide, swap=False):
    high = wide.astype(BF16)
    low = (wide - high.astype(F32)).astype(BF16)
    if swap:
        return jnp.dot(high, exact, preferred_element_type=F32) + jnp.dot(
            low, exact, preferred_element_type=F32
        )
    return jnp.dot(exact, high, preferred_element_type=F32) + jnp.dot(
        exact, low, preferred_element_type=F32
    )


def kernel(
    dims,
    q_ref, k_ref, v_ref, o_ref, arow_ref, acol_ref, ccol_ref, hgain_ref, wout_ref, res_ref,
    fgain_ref, up_ref, down_ref,
    mid_ref, mlp_ref,
    upw, dnw, ntok, act, psend, precv, msend, mrecv, cbuf, crecv, bsend, brecv, mixed, blockmem, st_out, st_in,
    w_send, w_recv, loc_sem, st_send, st_recv, c_send, c_recv, b_send, b_recv, t_send, t_recv, f_send,
    p_send, p_recv, m_send, m_recv,
):
    grp, sp, tp, heads, blocks, rows = dims
    g, z, t = lax.axis_index("grp"), lax.axis_index("sp"), lax.axis_index("tp")
    layer = grp * tp
    me = g * tp + t
    half = tp // 2
    same = grp * half
    core = lax.rem(t, 2)
    pair = t // 2
    place = g * half + pair
    mine = core * same + place
    partner = t + 1 - 2 * core
    counts = (upw.shape[1], dnw.shape[1])

    def there(gg, zz, tt):
        return {"grp": gg, "sp": zz, "tp": tt}

    barrier = pltpu.get_barrier_semaphore()
    for j in range(1, layer):
        d = lax.rem(me + j, layer)
        pl.semaphore_signal(
            barrier, inc=1, device_id=there(d // tp, z, lax.rem(d, tp)), device_id_type=MESH
        )

    @pl.when(z > 0)
    def _():
        pl.semaphore_signal(barrier, inc=1, device_id=there(g, z - 1, t), device_id_type=MESH)

    @pl.when(z < sp - 1)
    def _():
        pl.semaphore_signal(barrier, inc=1, device_id=there(g, z + 1, t), device_id_type=MESH)

    neighbours = (z + sp - 1) // sp + (2 * sp - 2 - z) // sp
    pl.semaphore_wait(barrier, layer - 1 + neighbours)

    hidden_half = up_ref.shape[1] // grp
    bufs = (upw, dnw)

    def own_piece(m, c):
        n = bufs[m].shape[2]
        if m == 0:
            return up_ref.at[
                pl.ds(c * n, n), pl.ds(pl.multiple_of(g * hidden_half, 128), hidden_half)
            ]
        n = bufs[m].shape[3]
        return down_ref.at[
            pl.ds(pl.multiple_of(g * hidden_half, 16), hidden_half), pl.ds(c * n, n)
        ]

    def weight_copy(m, c, origin, way, source=None):
        dst = bufs[m].at[origin, c]
        zz = z + 1 if way == 0 else z - 1
        return pltpu.make_async_remote_copy(
            src_ref=dst if source is None else source,
            dst_ref=dst,
            send_sem=w_send.at[m, way, origin, c],
            recv_sem=w_recv.at[m, origin, c],
            device_id=there(g, zz, t),
            device_id_type=MESH,
        )

    def local_copy(m, c):
        return pltpu.make_async_copy(own_piece(m, c), bufs[m].at[z, c], loc_sem.at[m, c])

    def start_own(m):
        for c in range(counts[m]):
            @pl.when(z < sp - 1)
            def _():
                weight_copy(m, c, z, 0, own_piece(m, c)).start()

            @pl.when(z > 0)
            def _():
                weight_copy(m, c, z, 1, own_piece(m, c)).start()

    def relay(m, s, c):
        left, right = z - 1 - s, z + 1 + s

        @pl.when(left >= 0)
        def _():
            weight_copy(m, c, left, 0).wait_recv()

            @pl.when(z < sp - 1)
            def _():
                weight_copy(m, c, left, 0).start()

        @pl.when(right < sp)
        def _():
            weight_copy(m, c, right, 1).wait_recv()

            @pl.when(z > 0)
            def _():
                weight_copy(m, c, right, 1).start()

    def relays(first, last):
        def body(s, _):
            for c in range(counts[0]):
                relay(0, s, c)
            return 0

        lax.fori_loop(first, last, body, 0)

    start_own(0)
    for m in range(2):
        for c in range(counts[m]):
            local_copy(m, c).start()

    scale = BLOCK ** (-0.5) if q_ref.shape[1] // heads == BLOCK else (q_ref.shape[1] // heads) ** (-0.5)
    dh = q_ref.shape[1] // heads
    totals, tails = {}, {}
    for h in range(heads):
        cols = pl.ds(h * dh, dh)
        run = None
        for b in range(blocks):
            at = pl.ds(b * BLOCK, BLOCK)
            cum = ccol_ref[at, h : h + 1]
            total = cum[BLOCK - 1 : BLOCK, :]
            tail = total + acol_ref[at, h : h + 1]
            tail_max = jnp.max(tail, axis=0, keepdims=True)
            weighted = v_ref[at, cols].astype(F32) * jnp.exp(tail - tail_max)
            key_t = k_ref[at, cols].astype(F32).T.astype(BF16)
            mem = split_dot(key_t, weighted) * scale
            blockmem[h, b] = mem
            totals[h, b], tails[h, b] = total, tail_max
            if run is None:
                run = (total, tail_max, mem)
            else:
                new = jnp.maximum(total + run[1], tail_max)
                run = (
                    total + run[0],
                    new,
                    jnp.exp(total + run[1] - new) * run[2] + jnp.exp(tail_max - new) * mem,
                )
        st_out[h, :dh, :] = run[2]
        st_out[h, dh : dh + 8, :] = jnp.broadcast_to(run[1], (8, dh))
        st_out[h, dh + 8 : dh + 16, :] = jnp.broadcast_to(run[0], (8, dh))

    def state_copy():
        return pltpu.make_async_remote_copy(
            src_ref=st_out,
            dst_ref=st_in,
            send_sem=st_send,
            recv_sem=st_recv,
            device_id=there(g, z + 1, t),
            device_id_type=MESH,
        )

    @pl.when(z == 0)
    def _():
        st_in[...] = jnp.zeros_like(st_in)

    @pl.when(z > 0)
    def _():
        state_copy().wait_recv()

    @pl.when(z < sp - 1)
    def _():
        for h in range(heads):
            m_in = st_in[h, dh : dh + 1, :]
            m_loc = st_out[h, dh : dh + 1, :]
            total = st_out[h, dh + 8 : dh + 9, :]
            new = jnp.maximum(total + m_in, m_loc)
            st_out[h, :dh, :] = (
                jnp.exp(total + m_in - new) * st_in[h, :dh, :]
                + jnp.exp(m_loc - new) * st_out[h, :dh, :]
            )
            st_out[h, dh : dh + 8, :] = jnp.broadcast_to(new, (8, dh))
        state_copy().start()

    third = (sp - 1) // 3
    relays(0, third)

    causal = lax.broadcasted_iota(jnp.int32, (BLOCK, BLOCK), 0) >= lax.broadcasted_iota(
        jnp.int32, (BLOCK, BLOCK), 1
    )
    gain = hgain_ref[...]
    for h in range(heads):
        cols = pl.ds(h * dh, dh)
        memory = st_in[h, :dh, :]
        stab = st_in[h, dh : dh + 1, 0:1]
        for b in range(blocks):
            at = pl.ds(b * BLOCK, BLOCK)
            cum = ccol_ref[at, h : h + 1]
            query = q_ref[at, cols]
            key_t = k_ref[at, cols].astype(F32).T.astype(BF16)
            log_weight = jnp.where(causal, cum + arow_ref[h * blocks + b : h * blocks + b + 1, :], NEG)
            carry = cum + stab
            row_max = jnp.maximum(jnp.max(log_weight, axis=1, keepdims=True), carry)
            scores = (
                jnp.dot(query, key_t, preferred_element_type=F32)
                * scale
                * jnp.exp(log_weight - row_max)
            )
            hidden = split_dot(v_ref[at, cols], scores, swap=True)
            hidden = hidden + jnp.exp(carry - row_max) * split_dot(query, memory)
            mean_sq = jnp.mean(hidden * hidden, axis=1, keepdims=True)
            gate = o_ref[at, cols].astype(F32)
            out = hidden * lax.rsqrt(mean_sq + EPS) * gain * (1.0 / (1.0 + jnp.exp(-gate)))
            mixed[at, cols] = out.astype(BF16)
            total, tail_max = totals[h, b], tails[h, b]
            new = jnp.maximum(total + stab, tail_max)
            memory = jnp.exp(total + stab - new) * memory + jnp.exp(tail_max - new) * blockmem[h, b]
            stab = new

    def cross_copy(q):
        return pltpu.make_async_remote_copy(
            src_ref=cbuf.at[q],
            dst_ref=crecv.at[q],
            send_sem=c_send.at[q],
            recv_sem=c_recv.at[q],
            device_id=there(g, z, partner),
            device_id_type=MESH,
        )

    def branch_copy(q, slot):
        return pltpu.make_async_remote_copy(
            src_ref=bsend.at[q],
            dst_ref=brecv.at[slot],
            send_sem=b_send.at[q],
            recv_sem=b_recv.at[slot],
            device_id=there(g, z, 2 * q + core),
            device_id_type=MESH,
        )

    def branch_part(d):
        return jnp.dot(
            mixed[pl.ds(pl.multiple_of(d * rows, rows), rows), :],
            wout_ref[...],
            preferred_element_type=F32,
        )

    for q in range(half):
        cbuf[q] = branch_part(2 * q + 1 - core).astype(BF16)
        cross_copy(q).start()
    for q in range(half):
        part = branch_part(2 * q + core)
        cross_copy(q).wait_recv()
        bsend[q] = (part + crecv[q].astype(F32)).astype(BF16)

        @pl.when(q != pair)
        def _():
            branch_copy(q, pair).start()

    brecv[pair] = bsend[pair]
    branch = res_ref[...].astype(F32)
    for q in range(half):
        @pl.when(q != pair)
        def _():
            branch_copy(q, q).wait_recv()

        branch = branch + brecv[q].astype(F32)
    mid = branch.astype(BF16)
    mid_ref[...] = mid
    wide = mid.astype(F32)
    mean_sq = jnp.mean(wide * wide, axis=1, keepdims=True)
    ntok[mine] = (wide * lax.rsqrt(mean_sq + EPS) * fgain_ref[...]).astype(BF16)

    def token_copy(j, slot):
        at = lax.rem(place + j, same)
        return pltpu.make_async_remote_copy(
            src_ref=ntok.at[slot],
            dst_ref=ntok.at[slot],
            send_sem=t_send.at[j],
            recv_sem=t_recv.at[slot],
            device_id=there(at // half, z, lax.rem(at, half) * 2 + core),
            device_id_type=MESH,
        )

    def partner_copy(j, side):
        slot = side * same + lax.rem(place + j, same)
        return pltpu.make_async_remote_copy(
            src_ref=ntok.at[slot],
            dst_ref=ntok.at[slot],
            send_sem=f_send.at[j],
            recv_sem=t_recv.at[slot],
            device_id=there(g, z, partner),
            device_id_type=MESH,
        )

    for j in range(1, same):
        token_copy(j, mine).start()
    partner_copy(0, core).start()
    relays(third, 2 * third)
    start_own(1)
    relays(2 * third, sp - 1)
    for c in range(counts[0]):
        local_copy(0, c).wait()

    width = ntok.shape[2]

    def up_half(side):
        def up_step(i, _):
            at = pl.ds(side * same + i * 2, 2)
            x = ntok[at].reshape(2 * rows, width)
            y = jnp.dot(x, upw[...].reshape(width, hidden_half), preferred_element_type=F32)
            y = jnp.maximum(y, 0.0)
            act[at] = (y * y).astype(BF16).reshape(2, rows, hidden_half)
            return 0

        lax.fori_loop(0, same // 2, up_step, 0)

    for j in range(1, same):
        token_copy(j, core * same + lax.rem(place + j, same)).wait_recv()
        partner_copy(j, core).start()
    up_half(core)
    for j in range(same):
        partner_copy(j, 1 - core).wait_recv()
    up_half(1 - core)
    for c in range(counts[1]):
        local_copy(1, c).wait()

    pieces = counts[1]

    def pre_copy(unit):
        return pltpu.make_async_remote_copy(
            src_ref=psend.at[unit],
            dst_ref=precv.at[unit],
            send_sem=p_send.at[unit],
            recv_sem=p_recv.at[unit],
            device_id=there(g, z, partner),
            device_id_type=MESH,
        )

    def mlp_copy(unit, p, slot):
        return pltpu.make_async_remote_copy(
            src_ref=msend.at[unit, p],
            dst_ref=mrecv.at[unit, slot],
            send_sem=m_send.at[unit, p],
            recv_sem=m_recv.at[unit, slot],
            device_id=there(p // half, z, 2 * (p % half) + core),
            device_id_type=MESH,
        )

    def down_piece(origin, c):
        unit = origin * pieces + c

        def product(side):
            x = act[pl.ds(side * same, same)].reshape(same * rows, hidden_half)
            return jnp.dot(x, dnw[origin, c], preferred_element_type=F32)

        psend[unit] = product(1 - core).astype(BF16).reshape(psend.shape[1:])
        pre_copy(unit).start()
        own = product(core).reshape(psend.shape[1:])
        pre_copy(unit).wait_recv()
        msend[unit] = (own + precv[unit].astype(F32)).astype(BF16)
        for p in range(same):
            @pl.when(p != place)
            def _():
                mlp_copy(unit, p, place).start()

    for c in range(pieces):
        down_piece(z, c)

    def down_step(s, _):
        for c in range(pieces):
            relay(1, s, c)

            @pl.when(z - 1 - s >= 0)
            def _():
                down_piece(z - 1 - s, c)

            @pl.when(z + 1 + s < sp)
            def _():
                down_piece(z + 1 + s, c)

        return 0

    lax.fori_loop(0, sp - 1, down_step, 0)

    def finish_unit(origin, c):
        unit = origin * pieces + c
        mrecv[unit, place] = msend[unit, place]
        total = jnp.zeros(mrecv.shape[2:], F32)
        for p in range(same):
            @pl.when(p != place)
            def _():
                mlp_copy(unit, p, p).wait_recv()

            total = total + mrecv[unit, p].astype(F32)
        n = mrecv.shape[3]
        mlp_ref[origin, :, c * n : (c + 1) * n] = total

    def finish_pair(s, _):
        @pl.when(z - s >= 0)
        def _():
            for c in range(pieces):
                finish_unit(z - s, c)

        @pl.when((s > 0) & (z + s < sp))
        def _():
            for c in range(pieces):
                finish_unit(z + s, c)

        return 0

    lax.fori_loop(0, sp, finish_pair, 0)

    def drain(origin, _):
        for c in range(pieces):
            unit = origin * pieces + c
            pre_copy(unit).wait_send()
            for p in range(same):
                @pl.when(p != place)
                def _():
                    mlp_copy(unit, p, place).wait_send()
        for m in range(2):
            for c in range(counts[m]):
                @pl.when((origin <= z) & (z < sp - 1))
                def _():
                    weight_copy(m, c, origin, 0).wait_send()

                @pl.when((origin >= z) & (z > 0))
                def _():
                    weight_copy(m, c, origin, 1).wait_send()
        return 0

    lax.fori_loop(0, sp, drain, 0)
    for q in range(half):
        cross_copy(q).wait_send()

        @pl.when(q != pair)
        def _():
            branch_copy(q, pair).wait_send()

    for j in range(1, same):
        token_copy(j, mine).wait_send()
    for j in range(same):
        partner_copy(j, core).wait_send()

    @pl.when(z < sp - 1)
    def _():
        state_copy().wait_send()


def shards(
    mesh_shape,
    queries, memory_keys, memory_values, output_preactivation, input_preactivation,
    forget_preactivation, extra_forget_terms, head_norm_gain, output_projection_matrix, residual,
    feedforward_norm_gain, feedforward_up_matrix, feedforward_down_matrix,
):
    grp, sp, tp = mesh_shape
    tokens = queries.shape[0]
    heads = input_preactivation.shape[0]
    blocks = tokens // BLOCK
    dh = queries.shape[1] // heads
    rows, width = residual.shape
    layer = grp * tp
    up_rows, hidden = feedforward_up_matrix.shape
    hidden_half = hidden // grp
    out_cols = feedforward_down_matrix.shape[1]
    chunks = 2
    pieces = 2 if out_cols % 256 == 0 else 1
    half = tp // 2
    same = grp * half
    units = sp * pieces

    log_forget = jax.nn.log_sigmoid(forget_preactivation) + extra_forget_terms
    cum = jnp.cumsum(log_forget.reshape(heads, blocks, BLOCK), axis=-1)
    rest = input_preactivation.reshape(heads, blocks, BLOCK) - cum
    arow = rest.reshape(heads * blocks, BLOCK)
    acol = rest.reshape(heads, tokens).T
    ccol = cum.reshape(heads, tokens).T

    vmem = pl.BlockSpec(memory_space=pltpu.VMEM)
    hbm = pl.BlockSpec(memory_space=pl.ANY)
    dma = pltpu.SemaphoreType.DMA
    mid, mlp = pl.pallas_call(
        functools.partial(kernel, (grp, sp, tp, heads, blocks, rows)),
        out_shape=(
            jax.ShapeDtypeStruct((rows, width), BF16),
            jax.ShapeDtypeStruct((sp, rows, out_cols), F32),
        ),
        in_specs=[vmem] * 11 + [hbm] * 2,
        out_specs=(vmem, vmem),
        scratch_shapes=[
            pltpu.VMEM((sp, chunks, up_rows // chunks, hidden_half), BF16),
            pltpu.VMEM((sp, pieces, hidden_half, out_cols // pieces), BF16),
            pltpu.VMEM((layer, rows, width), BF16),
            pltpu.VMEM((layer, rows, hidden_half), BF16),
            pltpu.VMEM((units, same, rows, out_cols // pieces), BF16),
            pltpu.VMEM((units, same, rows, out_cols // pieces), BF16),
            pltpu.VMEM((units, same, rows, out_cols // pieces), BF16),
            pltpu.VMEM((units, same, rows, out_cols // pieces), BF16),
            pltpu.VMEM((half, rows, width), BF16),
            pltpu.VMEM((half, rows, width), BF16),
            pltpu.VMEM((half, rows, width), BF16),
            pltpu.VMEM((half, rows, width), BF16),
            pltpu.VMEM((tokens, heads * dh), BF16),
            pltpu.VMEM((heads, blocks, dh, dh), F32),
            pltpu.VMEM((heads, dh + 16, dh), F32),
            pltpu.VMEM((heads, dh + 16, dh), F32),
            dma((2, 2, sp, chunks)),
            dma((2, sp, chunks)),
            dma((2, chunks)),
            dma,
            dma,
            dma((half,)),
            dma((half,)),
            dma((half,)),
            dma((half,)),
            dma((same,)),
            dma((layer,)),
            dma((same,)),
            dma((units,)),
            dma((units,)),
            dma((units, same)),
            dma((units, same)),
        ],
        compiler_params=pltpu.CompilerParams(
            collective_id=0, has_side_effects=True, vmem_limit_bytes=60 * 1024 * 1024
        ),
    )(
        queries, memory_keys, memory_values, output_preactivation, arow, acol, ccol,
        head_norm_gain.reshape(1, dh), output_projection_matrix, residual,
        feedforward_norm_gain.reshape(1, width), feedforward_up_matrix, feedforward_down_matrix,
    )
    mlp = mlp.transpose(1, 0, 2).reshape(rows, width)
    return (mid.astype(F32) + mlp).astype(BF16)


def solution(mesh):
    in_specs = (
        P(("grp", "sp"), "tp"),
        P(("grp", "sp"), "tp"),
        P(("grp", "sp"), "tp"),
        P(("grp", "sp"), "tp"),
        P("tp", ("grp", "sp")),
        P("tp", ("grp", "sp")),
        P("tp", ("grp", "sp")),
        P(),
        P("tp", None),
        P(("grp", "sp", "tp"), None),
        P(),
        P("sp", "tp"),
        P("tp", "sp"),
    )
    out_specs = P(("grp", "sp", "tp"), None)
    shape = (mesh.shape["grp"], mesh.shape["sp"], mesh.shape["tp"])
    return jax.shard_map(
        functools.partial(shards, shape),
        mesh=mesh,
        in_specs=in_specs,
        out_specs=out_specs,
        check_vma=False,
    )
```

```python
import functools

import jax
import jax.numpy as jnp
from jax import lax
from jax.experimental import pallas as pl
from jax.experimental.pallas import tpu as pltpu
from jax.sharding import PartitionSpec as P

BLOCK = 128
EPS = 1e-06
NEG = -1e30
MESH = pl.DeviceIdType.MESH
F32 = jnp.float32
BF16 = jnp.bfloat16


def split_dot(exact, wide, swap=False):
    high = wide.astype(BF16)
    low = (wide - high.astype(F32)).astype(BF16)
    if swap:
        return jnp.dot(high, exact, preferred_element_type=F32) + jnp.dot(
            low, exact, preferred_element_type=F32
        )
    return jnp.dot(exact, high, preferred_element_type=F32) + jnp.dot(
        exact, low, preferred_element_type=F32
    )


def kernel(
    dims,
    q_ref, k_ref, v_ref, o_ref, arow_ref, acol_ref, ccol_ref, hgain_ref, wout_ref, res_ref,
    fgain_ref, up_ref, down_ref,
    mid_ref, mlp_ref,
    upw, dnw, ntok, act, psend, precv, msend, mrecv, cbuf, crecv, bsend, brecv, mixed, blockmem, st_out, st_in,
    w_send, w_recv, loc_sem, st_send, st_recv, c_send, c_recv, b_send, b_recv, t_send, t_recv, f_send,
    p_send, p_recv, m_send, m_recv,
):
    grp, sp, tp, heads, blocks, rows = dims
    g, z, t = lax.axis_index("grp"), lax.axis_index("sp"), lax.axis_index("tp")
    layer = grp * tp
    me = g * tp + t
    half = tp // 2
    same = grp * half
    core = lax.rem(t, 2)
    pair = t // 2
    place = g * half + pair
    mine = core * same + place
    partner = t + 1 - 2 * core
    counts = (upw.shape[1], dnw.shape[1])

    def there(gg, zz, tt):
        return {"grp": gg, "sp": zz, "tp": tt}

    barrier = pltpu.get_barrier_semaphore()
    for j in range(1, layer):
        d = lax.rem(me + j, layer)
        pl.semaphore_signal(
            barrier, inc=1, device_id=there(d // tp, z, lax.rem(d, tp)), device_id_type=MESH
        )

    @pl.when(z > 0)
    def _():
        pl.semaphore_signal(barrier, inc=1, device_id=there(g, z - 1, t), device_id_type=MESH)

    @pl.when(z < sp - 1)
    def _():
        pl.semaphore_signal(barrier, inc=1, device_id=there(g, z + 1, t), device_id_type=MESH)

    neighbours = (z + sp - 1) // sp + (2 * sp - 2 - z) // sp
    pl.semaphore_wait(barrier, layer - 1 + neighbours)

    hidden_half = up_ref.shape[1] // grp
    bufs = (upw, dnw)

    def own_piece(m, c):
        n = bufs[m].shape[2]
        if m == 0:
            return up_ref.at[
                pl.ds(c * n, n), pl.ds(pl.multiple_of(g * hidden_half, 128), hidden_half)
            ]
        n = bufs[m].shape[3]
        return down_ref.at[
            pl.ds(pl.multiple_of(g * hidden_half, 16), hidden_half), pl.ds(c * n, n)
        ]

    def weight_copy(m, c, origin, way, source=None):
        dst = bufs[m].at[origin, c]
        zz = z + 1 if way == 0 else z - 1
        return pltpu.make_async_remote_copy(
            src_ref=dst if source is None else source,
            dst_ref=dst,
            send_sem=w_send.at[m, way, origin, c],
            recv_sem=w_recv.at[m, origin, c],
            device_id=there(g, zz, t),
            device_id_type=MESH,
        )

    def local_copy(m, c):
        return pltpu.make_async_copy(own_piece(m, c), bufs[m].at[z, c], loc_sem.at[m, c])

    def start_right(m, c):
        @pl.when(z < sp - 1)
        def _():
            weight_copy(m, c, z, 0, own_piece(m, c)).start()

    def start_left(m, c):
        @pl.when(z > 0)
        def _():
            weight_copy(m, c, z, 1, own_piece(m, c)).start()

    def relay(m, s, c):
        left, right = z - 1 - s, z + 1 + s

        @pl.when(left >= 0)
        def _():
            weight_copy(m, c, left, 0).wait_recv()

            @pl.when(z < sp - 1)
            def _():
                weight_copy(m, c, left, 0).start()

        @pl.when(right < sp)
        def _():
            weight_copy(m, c, right, 1).wait_recv()

            @pl.when(z > 0)
            def _():
                weight_copy(m, c, right, 1).start()

    def relays(first, last):
        def body(s, _):
            for c in range(counts[0]):
                relay(0, s, c)
            return 0

        lax.fori_loop(first, last, body, 0)

    start_right(0, 0)

    @pl.when(z > 1)
    def _():
        for c in range(1, counts[0]):
            start_right(0, c)

    for m in range(2):
        for c in range(counts[m]):
            start_left(m, c)
    for m in range(2):
        for c in range(counts[m]):
            local_copy(m, c).start()

    scale = BLOCK ** (-0.5) if q_ref.shape[1] // heads == BLOCK else (q_ref.shape[1] // heads) ** (-0.5)
    dh = q_ref.shape[1] // heads
    totals, tails = {}, {}
    for h in range(heads):
        cols = pl.ds(h * dh, dh)
        run = None
        for b in range(blocks):
            at = pl.ds(b * BLOCK, BLOCK)
            cum = ccol_ref[at, h : h + 1]
            total = cum[BLOCK - 1 : BLOCK, :]
            tail = total + acol_ref[at, h : h + 1]
            tail_max = jnp.max(tail, axis=0, keepdims=True)
            weighted = v_ref[at, cols].astype(F32) * jnp.exp(tail - tail_max)
            key_t = k_ref[at, cols].astype(F32).T.astype(BF16)
            mem = split_dot(key_t, weighted) * scale
            blockmem[h, b] = mem
            totals[h, b], tails[h, b] = total, tail_max
            if run is None:
                run = (total, tail_max, mem)
            else:
                new = jnp.maximum(total + run[1], tail_max)
                run = (
                    total + run[0],
                    new,
                    jnp.exp(total + run[1] - new) * run[2] + jnp.exp(tail_max - new) * mem,
                )
        st_out[h, :dh, :] = run[2]
        st_out[h, dh : dh + 8, :] = jnp.broadcast_to(run[1], (8, dh))
        st_out[h, dh + 8 : dh + 16, :] = jnp.broadcast_to(run[0], (8, dh))

    def state_copy():
        return pltpu.make_async_remote_copy(
            src_ref=st_out,
            dst_ref=st_in,
            send_sem=st_send,
            recv_sem=st_recv,
            device_id=there(g, z + 1, t),
            device_id_type=MESH,
        )

    @pl.when(z == 0)
    def _():
        st_in[...] = jnp.zeros_like(st_in)

    @pl.when(z > 0)
    def _():
        state_copy().wait_recv()

    @pl.when(z < sp - 1)
    def _():
        for h in range(heads):
            m_in = st_in[h, dh : dh + 1, :]
            m_loc = st_out[h, dh : dh + 1, :]
            total = st_out[h, dh + 8 : dh + 9, :]
            new = jnp.maximum(total + m_in, m_loc)
            st_out[h, :dh, :] = (
                jnp.exp(total + m_in - new) * st_in[h, :dh, :]
                + jnp.exp(m_loc - new) * st_out[h, :dh, :]
            )
            st_out[h, dh : dh + 8, :] = jnp.broadcast_to(new, (8, dh))
        state_copy().start()

    @pl.when(z <= 1)
    def _():
        for c in range(1, counts[0]):
            start_right(0, c)

    for c in range(counts[1]):
        start_right(1, c)

    third = (sp - 1) // 3
    relays(0, third)

    causal = lax.broadcasted_iota(jnp.int32, (BLOCK, BLOCK), 0) >= lax.broadcasted_iota(
        jnp.int32, (BLOCK, BLOCK), 1
    )
    gain = hgain_ref[...]
    for h in range(heads):
        cols = pl.ds(h * dh, dh)
        memory = st_in[h, :dh, :]
        stab = st_in[h, dh : dh + 1, 0:1]
        for b in range(blocks):
            at = pl.ds(b * BLOCK, BLOCK)
            cum = ccol_ref[at, h : h + 1]
            query = q_ref[at, cols]
            key_t = k_ref[at, cols].astype(F32).T.astype(BF16)
            log_weight = jnp.where(causal, cum + arow_ref[h * blocks + b : h * blocks + b + 1, :], NEG)
            carry = cum + stab
            row_max = jnp.maximum(jnp.max(log_weight, axis=1, keepdims=True), carry)
            scores = (
                jnp.dot(query, key_t, preferred_element_type=F32)
                * scale
                * jnp.exp(log_weight - row_max)
            )
            hidden = split_dot(v_ref[at, cols], scores, swap=True)
            hidden = hidden + jnp.exp(carry - row_max) * split_dot(query, memory)
            mean_sq = jnp.mean(hidden * hidden, axis=1, keepdims=True)
            gate = o_ref[at, cols].astype(F32)
            out = hidden * lax.rsqrt(mean_sq + EPS) * gain * (1.0 / (1.0 + jnp.exp(-gate)))
            mixed[at, cols] = out.astype(BF16)
            total, tail_max = totals[h, b], tails[h, b]
            new = jnp.maximum(total + stab, tail_max)
            memory = jnp.exp(total + stab - new) * memory + jnp.exp(tail_max - new) * blockmem[h, b]
            stab = new

    def cross_copy(q):
        return pltpu.make_async_remote_copy(
            src_ref=cbuf.at[q],
            dst_ref=crecv.at[q],
            send_sem=c_send.at[q],
            recv_sem=c_recv.at[q],
            device_id=there(g, z, partner),
            device_id_type=MESH,
        )

    def branch_copy(q, slot):
        return pltpu.make_async_remote_copy(
            src_ref=bsend.at[q],
            dst_ref=brecv.at[slot],
            send_sem=b_send.at[q],
            recv_sem=b_recv.at[slot],
            device_id=there(g, z, 2 * q + core),
            device_id_type=MESH,
        )

    def branch_part(d):
        return jnp.dot(
            mixed[pl.ds(pl.multiple_of(d * rows, rows), rows), :],
            wout_ref[...],
            preferred_element_type=F32,
        )

    for q in range(half):
        cbuf[q] = branch_part(2 * q + 1 - core).astype(BF16)
        cross_copy(q).start()
    for q in range(half):
        part = branch_part(2 * q + core)
        cross_copy(q).wait_recv()
        bsend[q] = (part + crecv[q].astype(F32)).astype(BF16)

        @pl.when(q != pair)
        def _():
            branch_copy(q, pair).start()

    brecv[pair] = bsend[pair]
    branch = res_ref[...].astype(F32)
    for q in range(half):
        @pl.when(q != pair)
        def _():
            branch_copy(q, q).wait_recv()

        branch = branch + brecv[q].astype(F32)
    mid = branch.astype(BF16)
    mid_ref[...] = mid
    wide = mid.astype(F32)
    mean_sq = jnp.mean(wide * wide, axis=1, keepdims=True)
    ntok[mine] = (wide * lax.rsqrt(mean_sq + EPS) * fgain_ref[...]).astype(BF16)

    def token_copy(j, slot):
        at = lax.rem(place + j, same)
        return pltpu.make_async_remote_copy(
            src_ref=ntok.at[slot],
            dst_ref=ntok.at[slot],
            send_sem=t_send.at[j],
            recv_sem=t_recv.at[slot],
            device_id=there(at // half, z, lax.rem(at, half) * 2 + core),
            device_id_type=MESH,
        )

    def partner_copy(j, side):
        slot = side * same + lax.rem(place + j, same)
        return pltpu.make_async_remote_copy(
            src_ref=ntok.at[slot],
            dst_ref=ntok.at[slot],
            send_sem=f_send.at[j],
            recv_sem=t_recv.at[slot],
            device_id=there(g, z, partner),
            device_id_type=MESH,
        )

    for j in range(1, same):
        token_copy(j, mine).start()
    partner_copy(0, core).start()
    relays(third, 2 * third)
    for c in range(counts[0]):
        local_copy(0, c).wait()

    width = ntok.shape[2]

    def up_half(side):
        def up_step(i, _):
            at = pl.ds(side * same + i * 2, 2)
            x = ntok[at].reshape(2 * rows, width)
            y = jnp.dot(x, upw[...].reshape(width, hidden_half), preferred_element_type=F32)
            y = jnp.maximum(y, 0.0)
            act[at] = (y * y).astype(BF16).reshape(2, rows, hidden_half)
            return 0

        lax.fori_loop(0, same // 2, up_step, 0)

    for j in range(1, same):
        token_copy(j, core * same + lax.rem(place + j, same)).wait_recv()
        partner_copy(j, core).start()
    relays(2 * third, sp - 1)
    for c in range(counts[1]):
        relay(1, 0, c)
    up_half(core)
    for j in range(same):
        partner_copy(j, 1 - core).wait_recv()
    up_half(1 - core)
    for c in range(counts[1]):
        local_copy(1, c).wait()

    pieces = counts[1]

    def pre_copy(unit):
        return pltpu.make_async_remote_copy(
            src_ref=psend.at[unit],
            dst_ref=precv.at[unit],
            send_sem=p_send.at[unit],
            recv_sem=p_recv.at[unit],
            device_id=there(g, z, partner),
            device_id_type=MESH,
        )

    def mlp_copy(unit, p, slot):
        return pltpu.make_async_remote_copy(
            src_ref=msend.at[unit, p],
            dst_ref=mrecv.at[unit, slot],
            send_sem=m_send.at[unit, p],
            recv_sem=m_recv.at[unit, slot],
            device_id=there(p // half, z, 2 * (p % half) + core),
            device_id_type=MESH,
        )

    def down_piece(origin, c):
        unit = origin * pieces + c

        def product(side):
            x = act[pl.ds(side * same, same)].reshape(same * rows, hidden_half)
            return jnp.dot(x, dnw[origin, c], preferred_element_type=F32)

        psend[unit] = product(1 - core).astype(BF16).reshape(psend.shape[1:])
        pre_copy(unit).start()
        own = product(core).reshape(psend.shape[1:])
        pre_copy(unit).wait_recv()
        msend[unit] = (own + precv[unit].astype(F32)).astype(BF16)
        for p in range(same):
            @pl.when(p != place)
            def _():
                mlp_copy(unit, p, place).start()

    for c in range(pieces):
        down_piece(z, c)

    def down_step(s, _):
        for c in range(pieces):
            @pl.when(s > 0)
            def _():
                relay(1, s, c)

            @pl.when(z - 1 - s >= 0)
            def _():
                down_piece(z - 1 - s, c)

            @pl.when(z + 1 + s < sp)
            def _():
                down_piece(z + 1 + s, c)

        return 0

    lax.fori_loop(0, sp - 1, down_step, 0)

    def finish_unit(origin, c):
        unit = origin * pieces + c
        mrecv[unit, place] = msend[unit, place]
        total = jnp.zeros(mrecv.shape[2:], F32)
        for p in range(same):
            @pl.when(p != place)
            def _():
                mlp_copy(unit, p, p).wait_recv()

            total = total + mrecv[unit, p].astype(F32)
        n = mrecv.shape[3]
        mlp_ref[origin, :, c * n : (c + 1) * n] = total

    def finish_pair(s, _):
        @pl.when(z - s >= 0)
        def _():
            for c in range(pieces):
                finish_unit(z - s, c)

        @pl.when((s > 0) & (z + s < sp))
        def _():
            for c in range(pieces):
                finish_unit(z + s, c)

        return 0

    lax.fori_loop(0, sp, finish_pair, 0)

    def drain(origin, _):
        for c in range(pieces):
            unit = origin * pieces + c
            pre_copy(unit).wait_send()
            for p in range(same):
                @pl.when(p != place)
                def _():
                    mlp_copy(unit, p, place).wait_send()
        for m in range(2):
            for c in range(counts[m]):
                @pl.when((origin <= z) & (z < sp - 1))
                def _():
                    weight_copy(m, c, origin, 0).wait_send()

                @pl.when((origin >= z) & (z > 0))
                def _():
                    weight_copy(m, c, origin, 1).wait_send()
        return 0

    lax.fori_loop(0, sp, drain, 0)
    for q in range(half):
        cross_copy(q).wait_send()

        @pl.when(q != pair)
        def _():
            branch_copy(q, pair).wait_send()

    for j in range(1, same):
        token_copy(j, mine).wait_send()
    for j in range(same):
        partner_copy(j, core).wait_send()

    @pl.when(z < sp - 1)
    def _():
        state_copy().wait_send()


def shards(
    mesh_shape,
    queries, memory_keys, memory_values, output_preactivation, input_preactivation,
    forget_preactivation, extra_forget_terms, head_norm_gain, output_projection_matrix, residual,
    feedforward_norm_gain, feedforward_up_matrix, feedforward_down_matrix,
):
    grp, sp, tp = mesh_shape
    tokens = queries.shape[0]
    heads = input_preactivation.shape[0]
    blocks = tokens // BLOCK
    dh = queries.shape[1] // heads
    rows, width = residual.shape
    layer = grp * tp
    up_rows, hidden = feedforward_up_matrix.shape
    hidden_half = hidden // grp
    out_cols = feedforward_down_matrix.shape[1]
    chunks = 2
    pieces = 2 if out_cols % 256 == 0 else 1
    half = tp // 2
    same = grp * half
    units = sp * pieces

    log_forget = jax.nn.log_sigmoid(forget_preactivation) + extra_forget_terms
    cum = jnp.cumsum(log_forget.reshape(heads, blocks, BLOCK), axis=-1)
    rest = input_preactivation.reshape(heads, blocks, BLOCK) - cum
    arow = rest.reshape(heads * blocks, BLOCK)
    acol = rest.reshape(heads, tokens).T
    ccol = cum.reshape(heads, tokens).T

    vmem = pl.BlockSpec(memory_space=pltpu.VMEM)
    hbm = pl.BlockSpec(memory_space=pl.ANY)
    dma = pltpu.SemaphoreType.DMA
    mid, mlp = pl.pallas_call(
        functools.partial(kernel, (grp, sp, tp, heads, blocks, rows)),
        out_shape=(
            jax.ShapeDtypeStruct((rows, width), BF16),
            jax.ShapeDtypeStruct((sp, rows, out_cols), F32),
        ),
        in_specs=[vmem] * 11 + [hbm] * 2,
        out_specs=(vmem, vmem),
        scratch_shapes=[
            pltpu.VMEM((sp, chunks, up_rows // chunks, hidden_half), BF16),
            pltpu.VMEM((sp, pieces, hidden_half, out_cols // pieces), BF16),
            pltpu.VMEM((layer, rows, width), BF16),
            pltpu.VMEM((layer, rows, hidden_half), BF16),
            pltpu.VMEM((units, same, rows, out_cols // pieces), BF16),
            pltpu.VMEM((units, same, rows, out_cols // pieces), BF16),
            pltpu.VMEM((units, same, rows, out_cols // pieces), BF16),
            pltpu.VMEM((units, same, rows, out_cols // pieces), BF16),
            pltpu.VMEM((half, rows, width), BF16),
            pltpu.VMEM((half, rows, width), BF16),
            pltpu.VMEM((half, rows, width), BF16),
            pltpu.VMEM((half, rows, width), BF16),
            pltpu.VMEM((tokens, heads * dh), BF16),
            pltpu.VMEM((heads, blocks, dh, dh), F32),
            pltpu.VMEM((heads, dh + 16, dh), F32),
            pltpu.VMEM((heads, dh + 16, dh), F32),
            dma((2, 2, sp, chunks)),
            dma((2, sp, chunks)),
            dma((2, chunks)),
            dma,
            dma,
            dma((half,)),
            dma((half,)),
            dma((half,)),
            dma((half,)),
            dma((same,)),
            dma((layer,)),
            dma((same,)),
            dma((units,)),
            dma((units,)),
            dma((units, same)),
            dma((units, same)),
        ],
        compiler_params=pltpu.CompilerParams(
            collective_id=0, has_side_effects=True, vmem_limit_bytes=60 * 1024 * 1024
        ),
    )(
        queries, memory_keys, memory_values, output_preactivation, arow, acol, ccol,
        head_norm_gain.reshape(1, dh), output_projection_matrix, residual,
        feedforward_norm_gain.reshape(1, width), feedforward_up_matrix, feedforward_down_matrix,
    )
    mlp = mlp.transpose(1, 0, 2).reshape(rows, width)
    return (mid.astype(F32) + mlp).astype(BF16)


def solution(mesh):
    in_specs = (
        P(("grp", "sp"), "tp"),
        P(("grp", "sp"), "tp"),
        P(("grp", "sp"), "tp"),
        P(("grp", "sp"), "tp"),
        P("tp", ("grp", "sp")),
        P("tp", ("grp", "sp")),
        P("tp", ("grp", "sp")),
        P(),
        P("tp", None),
        P(("grp", "sp", "tp"), None),
        P(),
        P("sp", "tp"),
        P("tp", "sp"),
    )
    out_specs = P(("grp", "sp", "tp"), None)
    shape = (mesh.shape["grp"], mesh.shape["sp"], mesh.shape["tp"])
    return jax.shard_map(
        functools.partial(shards, shape),
        mesh=mesh,
        in_specs=in_specs,
        out_specs=out_specs,
        check_vma=False,
    )
```
